256 devices in a mesh: grp: 2 (over y), sp: 16 (over z), tp: 8 (over x, core).
Axes of the slice: x: 4, y: 2, z: 16, core: 2. Of those that a mesh axis runs over, the one named last changes fastest.
The devices are a block of a 4x16x16 slice.
Arguments:
- hidden_in: bfloat16 [12288, 4096], P(('grp', 'sp'), 'tp'), parts along dimension 0, may hold values from -30 to 30
- in_gain: float32 [2, 4096], P(None, 'tp'), may hold values from 0.1 to 1.9
- w_value: bfloat16 [2, 4096, 2048], P(None, 'sp', 'tp'), may hold values from -0.09375 to 0.09375
- w_gate: bfloat16 [2, 4096, 2048], P(None, 'sp', 'tp'), may hold values from -0.09375 to 0.09375
- conv_taps: float32 [2, 31, 2048], P(None, None, 'tp'), may hold values from -9 to 9
- norm_gain: float32 [2, 2048], P(None, 'tp'), may hold values from 0.1 to 1.9
- norm_shift: float32 [2, 2048], P(None, 'tp'), may hold values from -3 to 3
- w_out: bfloat16 [2, 2048, 4096], P(None, 'tp', 'sp'), may hold values from -0.125 to 0.125
Outputs:
- hidden_out: bfloat16 [12288, 4096], P(('grp', 'sp'), 'tp'), parts along dimension 0
The draws below stay inside these ranges and needn't reach their ends.
There are 2 independent parts, one for each index of `grp`. The reference program is written for one: setup_inputs(seed, part) draws one part's arguments, and reference() takes and returns one part's arrays. A program takes and returns all parts, laid end to end along the dimension named above; an argument that names none is the same for every part. Nothing has to cross between parts.
All inputs are finite; a program needn't handle non-finite values.
Results may differ from the reference program's by a relative error of at most 0.013.
Values may be sent and summed in bfloat16 or wider, within the bound.
No kernel may reach another device: no remote copies, remote signals or barrier semaphores. Data moves between devices by JAX's collectives and lax.ppermute only.
A program may use at most 64 MiB of HBM per device.

```python
import math
import jax
import jax.numpy as jnp
from jax import lax

D = 4096
C = 2048
KERNEL = 31
LAYERS = 2
TOKENS = 6144
N_TP = 8


def draw_hidden_in(key, part):
    keys = jax.random.split(key, 3)
    base = jnp.clip(jax.random.normal(keys[0], (TOKENS, D), jnp.float32), -4.0, 4.0)
    ramp = 3.0 ** (jnp.arange(D, dtype=jnp.float32) / D - 0.5)
    column = ramp * jnp.exp(jax.random.uniform(keys[1], (D,), jnp.float32, math.log(0.6), math.log(1.6)))
    row_scale = jnp.exp(jax.random.uniform(keys[2], (TOKENS,), jnp.float32, math.log(0.4), math.log(2.5)))
    return (base * row_scale[:, None] * column[None, :]).astype(jnp.bfloat16)


def draw_conv_taps(key, part):
    keys = jax.random.split(key, 2)
    base = jnp.clip(jax.random.normal(keys[0], (LAYERS, KERNEL, C), jnp.float32), -4.0, 4.0)
    ramp = 3.0 ** (jnp.arange(C, dtype=jnp.float32) / C)
    channel = ramp * jnp.exp(jax.random.uniform(keys[1], (C,), jnp.float32, 0.0, math.log(4.0)))
    return base / math.sqrt(KERNEL) * channel[None, None, :]


def block_levels(own_key, extent, pieces, smallest, largest):
    level, own = 1.0, jax.random.fold_in(own_key, 6)
    for axis_at, parts in pieces:
        heights = jnp.exp(jax.random.uniform(jax.random.fold_in(own, axis_at), (parts,), jnp.float32, smallest / len(pieces), largest / len(pieces)))
        level = level * jnp.repeat(heights, extent[axis_at] // parts).reshape([-1 if axis == axis_at else 1 for axis in range(len(extent))])
    return level


def scatter_about(own_key, shape, spread, most, cuts=(), kind=jnp.bfloat16):
    drawn = spread * jax.random.normal(own_key, shape, jnp.float32)
    if cuts:
        drawn = drawn * block_levels(own_key, shape, cuts, -0.22, 0.18)
    return jnp.clip(drawn, -most, most).astype(kind)


def setup_inputs(seed: int = 0, part: int = 0) -> dict:
    key_of = jax.random.split(jax.random.key(seed), 9)
    own_keys = jax.random.split(jax.random.fold_in(key_of[8], part), 9)
    return {
        "hidden_in": draw_hidden_in(jax.random.fold_in(jax.random.fold_in(key_of[8], part), 71), part),
        "in_gain": jnp.clip(1.0 + 0.18 * jax.random.normal(key_of[1], (LAYERS, D), jnp.float32), 0.1, 1.9),
        "w_value": scatter_about(key_of[2], (LAYERS, D, C), D ** -0.5, 0.09375, ((1, 16), (2, 8))),
        "w_gate": scatter_about(key_of[3], (LAYERS, D, C), D ** -0.5, 0.09375, ((1, 16), (2, 8))),
        "conv_taps": draw_conv_taps(jax.random.fold_in(key_of[8], 71), part),
        "norm_gain": jnp.clip(1.0 + 0.18 * jax.random.normal(key_of[5], (LAYERS, C), jnp.float32), 0.1, 1.9),
        "norm_shift": scatter_about(key_of[6], (LAYERS, C), 0.5, 3.0, ((1, 8),), jnp.float32),
        "w_out": scatter_about(key_of[7], (LAYERS, C, D), C ** -0.5, 0.125, ((1, 8), (2, 16))),
    }


epsilon = 1e-06

def block_sum(mixed_out, weight):
    block_width = C // N_TP

    def add_block(block_index, running):
        offset = block_index.astype(jnp.int32) * block_width
        block_cols = lax.dynamic_slice_in_dim(mixed_out, offset, block_width, 1)
        block_rows = lax.dynamic_slice_in_dim(weight, offset, block_width, 0)
        partial_value = jnp.dot(block_cols, block_rows, preferred_element_type=jnp.float32).astype(jnp.bfloat16)
        partial_value = lax.optimization_barrier(partial_value)
        return running + partial_value.astype(jnp.float32)
    start_sum = jnp.zeros((mixed_out.shape[0], weight.shape[1]), jnp.float32)
    return lax.fori_loop(0, N_TP, add_block, start_sum)

def causal_taps(gated_wide, taps):
    row_total = gated_wide.shape[0]
    padded = jnp.concatenate([jnp.zeros((KERNEL - 1, gated_wide.shape[1]), jnp.float32), gated_wide], axis=0)

    def add_tap(tap_index, running):
        where = tap_index.astype(jnp.int32)
        window = lax.dynamic_slice_in_dim(padded, where, row_total, 0)
        weight_row = lax.dynamic_slice_in_dim(taps, where, 1, 0)
        return running + weight_row * window
    start_sum = jnp.zeros(gated_wide.shape, jnp.float32)
    return lax.fori_loop(0, KERNEL, add_tap, start_sum)

def reference(hidden_in, in_gain, w_value, w_gate, conv_taps, norm_gain, norm_shift, w_out):
    hidden = hidden_in
    for layer_idx in range(LAYERS):
        widened = hidden.astype(jnp.float32)
        inv_rms = lax.rsqrt(lax.optimization_barrier(jnp.mean(widened * widened, axis=1, keepdims=True)) + epsilon)
        normalized = (widened * inv_rms * in_gain[layer_idx]).astype(jnp.bfloat16)
        value_part = jnp.dot(normalized, w_value[layer_idx], preferred_element_type=jnp.float32)
        gate_part = jnp.dot(normalized, w_gate[layer_idx], preferred_element_type=jnp.float32)
        gated = (value_part * jax.nn.sigmoid(gate_part)).astype(jnp.bfloat16)
        conved = causal_taps(gated.astype(jnp.float32), conv_taps[layer_idx])
        row_mean = lax.optimization_barrier(jnp.mean(conved, axis=1, keepdims=True))
        variance = lax.optimization_barrier(jnp.mean(jnp.square(conved - row_mean), axis=1, keepdims=True))
        normed = (conved - row_mean) * lax.rsqrt(variance + epsilon) * norm_gain[layer_idx] + norm_shift[layer_idx]
        mixed_out = jax.nn.silu(normed).astype(jnp.bfloat16)
        branch = block_sum(mixed_out, w_out[layer_idx])
        hidden = (hidden.astype(jnp.float32) + branch).astype(jnp.bfloat16)
    return hidden
```

```python
import jax
import jax.numpy as jnp
from jax import lax
from jax.experimental import pallas as pl
from jax.experimental.pallas import tpu as pltpu
from jax.sharding import PartitionSpec as P

epsilon = 1e-06


def shifted(value, axis, steps):
    count = lax.axis_size(axis)
    return lax.ppermute(value, axis, [(i, (i + steps) % count) for i in range(count)])


def swapped(value):
    return lax.ppermute(value, "tp", [(i, i ^ 1) for i in range(lax.axis_size("tp"))])


def passed_along(value, axis, steps):
    count = lax.axis_size(axis)
    initial, last = (max(0, -steps), min(count, count - steps))
    return lax.ppermute(value, axis, [(source, source + steps) for source in range(initial, last)])


def offsets_of(count):
    half = count // 2
    apart = [d if d <= half else d - count for d in range(0, count, 2)]
    return sorted(apart, key=lambda d: -abs(d))


def project(pieces, inv_rms, rows, width):
    tokens, size = pieces[0].shape
    count = len(pieces)
    offsets = offsets_of(count)[::-1]

    def kernel(*refs):
        blocks, (inv_ref, w_ref, out_ref, held, arrived) = refs[:count], refs[count:]
        lane = lax.axis_index("tp")
        other = lane + 1 - 2 * (lane % 2)
        copies = []
        for i in range(count):
            base = lane if i < len(offsets) else other
            at = (base + offsets[i % len(offsets)] + count) % count
            copies.append(
                pltpu.make_async_copy(
                    w_ref.at[pl.ds(pl.multiple_of(at * size, size), size), pl.ds(0, 2 * width)],
                    held.at[i],
                    arrived.at[i],
                )
            )
            copies[-1].start()
        total = None
        for i in range(count):
            copies[i].wait()
            part = jnp.dot(blocks[i][...], held[i], preferred_element_type=jnp.float32)
            total = part if total is None else total + part
        inv = inv_ref[...]
        value, gate = total[:, :width] * inv, total[:, width:] * inv
        out_ref[...] = (value * jax.nn.sigmoid(gate)).astype(out_ref.dtype)

    whole = pl.BlockSpec(memory_space=pltpu.VMEM)
    return pl.pallas_call(
        kernel,
        out_shape=jax.ShapeDtypeStruct((tokens, width), jnp.bfloat16),
        in_specs=[whole] * (count + 1) + [pl.BlockSpec(memory_space=pl.ANY)],
        out_specs=whole,
        scratch_shapes=[
            pltpu.VMEM((count, size, 2 * width), jnp.bfloat16),
            pltpu.SemaphoreType.DMA((count,)),
        ],
        compiler_params=pltpu.CompilerParams(vmem_limit_bytes=24 << 20),
        cost_estimate=pl.CostEstimate(
            flops=4 * tokens * size * count * width,
            bytes_accessed=4 * size * count * width,
            transcendentals=tokens * width,
        ),
        name="project",
    )(*pieces, inv_rms, rows)


def depthwise(gated, before, taps):
    tokens, width = gated.shape
    reach = taps.shape[0] - 1
    lead = -(-reach // 8) * 8
    tile = 64
    lanes = 128

    def kernel(gated_ref, before_ref, taps_ref, out_ref, wide):
        wide[pl.ds(0, lead), :] = jnp.concatenate(
            [
                jnp.zeros((lead - reach, width), jnp.float32),
                before_ref[...].astype(jnp.float32),
            ],
            axis=0,
        )
        wide[pl.ds(lead, tokens), :] = gated_ref[...].astype(jnp.float32)
        for start in range(0, tokens, tile):
            for lane in range(0, width, lanes):
                total = None
                for k in range(reach + 1):
                    window = wide[pl.ds(start + lead - reach + k, tile), pl.ds(lane, lanes)]
                    part = taps_ref[pl.ds(k, 1), pl.ds(lane, lanes)] * window
                    total = part if total is None else total + part
                out_ref[pl.ds(start, tile), pl.ds(lane, lanes)] = total

    whole = pl.BlockSpec(memory_space=pltpu.VMEM)
    return pl.pallas_call(
        kernel,
        out_shape=jax.ShapeDtypeStruct((tokens, width), jnp.float32),
        in_specs=[whole] * 3,
        out_specs=whole,
        scratch_shapes=[pltpu.VMEM((lead + tokens, width), jnp.float32)],
        compiler_params=pltpu.CompilerParams(vmem_limit_bytes=8 << 20),
        cost_estimate=pl.CostEstimate(
            flops=2 * tokens * width * (reach + 1),
            bytes_accessed=6 * tokens * width,
            transcendentals=0,
        ),
        name="depthwise",
    )(gated, before, taps)


def shares(mixed, held, fetched, across=None):
    tokens, width = mixed.shape
    tp = lax.axis_size("tp")
    offsets = offsets_of(tp)
    count = len(offsets)
    size = held.shape[0] // tp
    last = [] if across is None else [jax.ShapeDtypeStruct((tokens, size), jnp.float32)]
    outs = [jax.ShapeDtypeStruct((tokens, size), jnp.bfloat16)] * (count - len(last)) + last

    def kernel(mixed_ref, held_ref, fetched_ref, *refs):
        arrived, out_refs = refs[: len(refs) - count], refs[len(refs) - count :]
        lane = lax.axis_index("tp")
        base = lane if arrived else lane + 1 - 2 * (lane % 2)
        odd = lax.axis_index("grp") % 2 == 1
        for i, d in enumerate(offsets):
            for j in range(0, size, width):
                at = pl.multiple_of((base + d + tp) % tp * size + j, width)
                block = held_ref[pl.ds(at, width), :]
                pair = fetched_ref[pl.ds(at, width), :]
                block = jnp.concatenate(
                    [jnp.where(odd, pair, block), jnp.where(odd, block, pair)], axis=1
                )
                part = jnp.dot(mixed_ref[...], block, preferred_element_type=jnp.float32)
                if arrived:
                    part += arrived[i][:, pl.ds(j, width)].astype(jnp.float32)
                out_refs[i][:, pl.ds(j, width)] = part.astype(out_refs[i].dtype)

    whole = pl.BlockSpec(memory_space=pltpu.VMEM)
    given = [] if across is None else across
    return pl.pallas_call(
        kernel,
        out_shape=outs,
        in_specs=[whole] * (3 + len(given)),
        out_specs=[whole] * count,
        compiler_params=pltpu.CompilerParams(vmem_limit_bytes=16 << 20),
        cost_estimate=pl.CostEstimate(
            flops=2 * tokens * width * size * count,
            bytes_accessed=4 * tokens * size * count,
            transcendentals=0,
        ),
        name="shares",
    )(mixed, held, fetched, *given)


def over_lanes(part):
    pair = part + swapped(part)
    return sum((shifted(pair, "tp", d) for d in offsets_of(lax.axis_size("tp"))[:-1]), pair)


def fetched_rows(held):
    return lax.ppermute(held, "grp", [(i, i ^ 1) for i in range(lax.axis_size("grp"))])


def shards(hidden_in, in_gain, w_value, w_gate, conv_taps, norm_gain, norm_shift, w_out):
    layer_count = w_value.shape[0]
    reach_rows = conv_taps.shape[1] - 1
    tp = lax.axis_size("tp")
    tokens = hidden_in.shape[0]
    features = hidden_in.shape[1] * tp
    width = w_value.shape[2]
    channels = width * tp
    offsets = offsets_of(tp)

    half = w_out.shape[2] // 2
    mine = lax.axis_index("grp") % 2 * half
    taken = []
    for layer in range(layer_count):
        part = lax.dynamic_slice_in_dim(w_out[layer], mine, half, 1)
        rows = jnp.concatenate([w_value[layer], w_gate[layer], part], axis=1)
        taken.append(lax.all_gather(rows, "sp", axis=0, tiled=True))

    def run(layer, current):
        held = taken[layer][:, 2 * width :]
        fetched = fetched_rows(held)
        widened = current.astype(jnp.float32)
        squares = over_lanes(jnp.sum(widened * widened, axis=1))
        scaled = (widened * in_gain[layer]).astype(jnp.bfloat16)
        near = [scaled if d == 0 else shifted(scaled, "tp", -d) for d in offsets]
        inv_rms = lax.rsqrt(squares / features + epsilon)[:, None]
        far = [swapped(piece) for piece in near]
        gated = project(near[::-1] + far[::-1], inv_rms, taken[layer], width)
        before = passed_along(gated[tokens - reach_rows :], "sp", 1)
        conved = depthwise(gated, before, conv_taps[layer])
        sums = jnp.stack([jnp.sum(conved, axis=1), jnp.sum(conved * conved, axis=1)])
        totals = over_lanes(sums)
        row_mean = totals[0] / channels
        spread = totals[1] / channels - row_mean * row_mean
        normed = (conved - row_mean[:, None]) * lax.rsqrt(spread + epsilon)[:, None] * norm_gain[
            layer
        ] + norm_shift[layer]
        mixed_out = jax.nn.silu(normed).astype(jnp.bfloat16)
        across = [swapped(piece) for piece in shares(mixed_out, held, fetched)]
        pairs = shares(mixed_out, held, fetched, across)
        summed = widened + pairs[-1]
        for piece, d in zip(pairs[:-1], offsets):
            summed += shifted(piece, "tp", d).astype(jnp.float32)
        return summed.astype(jnp.bfloat16)

    current = hidden_in
    for layer in range(layer_count):
        current = run(layer, current)
    return current


def solution(mesh):
    placed = (
        P(("grp", "sp"), "tp"),
        P(None, "tp"),
        P(None, "sp", "tp"),
        P(None, "sp", "tp"),
        P(None, None, "tp"),
        P(None, "tp"),
        P(None, "tp"),
        P(None, "tp", "sp"),
    )
    return jax.shard_map(
        shards, mesh=mesh, in_specs=placed, out_specs=P(("grp", "sp"), "tp"), check_vma=False
    )
```

```python
import jax
import jax.numpy as jnp
from jax import lax
from jax.experimental import pallas as pl
from jax.experimental.pallas import tpu as pltpu
from jax.sharding import PartitionSpec as P

epsilon = 1e-06


def shifted(value, axis, steps):
    count = lax.axis_size(axis)
    return lax.ppermute(value, axis, [(i, (i + steps) % count) for i in range(count)])


def swapped(value):
    return lax.ppermute(value, "tp", [(i, i ^ 1) for i in range(lax.axis_size("tp"))])


def passed_along(value, axis, steps):
    count = lax.axis_size(axis)
    initial, last = (max(0, -steps), min(count, count - steps))
    return lax.ppermute(value, axis, [(source, source + steps) for source in range(initial, last)])


def offsets_of(count):
    half = count // 2
    apart = [d if d <= half else d - count for d in range(0, count, 2)]
    return sorted(apart, key=lambda d: -abs(d))


def project(pieces, inv_rms, rows, width):
    tokens, size = pieces[0].shape
    count = len(pieces)
    offsets = offsets_of(count)[::-1]

    def kernel(*refs):
        blocks, (inv_ref, w_ref, out_ref, held, arrived) = refs[:count], refs[count:]
        lane = lax.axis_index("tp")
        other = lane + 1 - 2 * (lane % 2)
        copies = []
        for i in range(count):
            base = lane if i < len(offsets) else other
            at = (base + offsets[i % len(offsets)] + count) % count
            copies.append(
                pltpu.make_async_copy(
                    w_ref.at[pl.ds(pl.multiple_of(at * size, size), size), pl.ds(0, 2 * width)],
                    held.at[i],
                    arrived.at[i],
                )
            )
            copies[-1].start()
        total = None
        for i in range(count):
            copies[i].wait()
            part = jnp.dot(blocks[i][...], held[i], preferred_element_type=jnp.float32)
            total = part if total is None else total + part
        inv = inv_ref[...]
        value, gate = total[:, :width] * inv, total[:, width:] * inv
        out_ref[...] = (value * jax.nn.sigmoid(gate)).astype(out_ref.dtype)

    whole = pl.BlockSpec(memory_space=pltpu.VMEM)
    return pl.pallas_call(
        kernel,
        out_shape=jax.ShapeDtypeStruct((tokens, width), jnp.bfloat16),
        in_specs=[whole] * (count + 1) + [pl.BlockSpec(memory_space=pl.ANY)],
        out_specs=whole,
        scratch_shapes=[
            pltpu.VMEM((count, size, 2 * width), jnp.bfloat16),
            pltpu.SemaphoreType.DMA((count,)),
        ],
        compiler_params=pltpu.CompilerParams(vmem_limit_bytes=24 << 20),
        cost_estimate=pl.CostEstimate(
            flops=4 * tokens * size * count * width,
            bytes_accessed=4 * size * count * width,
            transcendentals=tokens * width,
        ),
        name="project",
    )(*pieces, inv_rms, rows)


def depthwise(gated, taps, lead):
    total_rows, width = gated.shape
    tokens = total_rows - lead
    reach = taps.shape[0] - 1
    tile = 32
    lanes = 128

    def kernel(gated_ref, taps_ref, out_ref, wide):
        wide[...] = gated_ref[...].astype(jnp.float32)

        @pl.loop(0, tokens // tile)
        def _(index):
            start = pl.multiple_of(index * tile, tile)
            for lane in range(0, width, lanes):
                rows = wide[pl.ds(start, tile + lead), pl.ds(lane, lanes)]
                total = None
                for k in range(reach + 1):
                    first = lead - reach + k
                    window = lax.slice_in_dim(rows, first, first + tile, axis=0)
                    part = taps_ref[pl.ds(k, 1), pl.ds(lane, lanes)] * window
                    total = part if total is None else total + part
                out_ref[pl.ds(start, tile), pl.ds(lane, lanes)] = total

    whole = pl.BlockSpec(memory_space=pltpu.VMEM)
    return pl.pallas_call(
        kernel,
        out_shape=jax.ShapeDtypeStruct((tokens, width), jnp.float32),
        in_specs=[whole] * 2,
        out_specs=whole,
        scratch_shapes=[pltpu.VMEM((total_rows, width), jnp.float32)],
        compiler_params=pltpu.CompilerParams(vmem_limit_bytes=8 << 20),
        cost_estimate=pl.CostEstimate(
            flops=2 * tokens * width * (reach + 1),
            bytes_accessed=6 * tokens * width,
            transcendentals=0,
        ),
        name="depthwise",
    )(gated, taps)


def shares(mixed, held, fetched, across=None):
    tokens, width = mixed.shape
    tp = lax.axis_size("tp")
    offsets = offsets_of(tp)
    count = len(offsets)
    size = held.shape[0] // tp
    last = [] if across is None else [jax.ShapeDtypeStruct((tokens, size), jnp.float32)]
    outs = [jax.ShapeDtypeStruct((count - len(last), tokens, size), jnp.bfloat16)] + last

    def kernel(mixed_ref, held_ref, fetched_ref, *refs):
        arrived, (pairs_ref, *own_ref) = refs[: len(refs) - len(outs)], refs[len(refs) - len(outs) :]
        lane = lax.axis_index("tp")
        base = lane if arrived else lane + 1 - 2 * (lane % 2)
        odd = lax.axis_index("grp") % 2 == 1
        for i, d in enumerate(offsets):
            for j in range(0, size, width):
                at = pl.multiple_of((base + d + tp) % tp * size + j, width)
                block = held_ref[pl.ds(at, width), :]
                pair = fetched_ref[pl.ds(at, width), :]
                block = jnp.concatenate(
                    [jnp.where(odd, pair, block), jnp.where(odd, block, pair)], axis=1
                )
                part = jnp.dot(mixed_ref[...], block, preferred_element_type=jnp.float32)
                if arrived:
                    part += arrived[0][i, :, pl.ds(j, width)].astype(jnp.float32)
                if arrived and d == 0:
                    own_ref[0][:, pl.ds(j, width)] = part
                else:
                    pairs_ref[i, :, pl.ds(j, width)] = part.astype(jnp.bfloat16)

    whole = pl.BlockSpec(memory_space=pltpu.VMEM)
    given = [] if across is None else [across]
    return pl.pallas_call(
        kernel,
        out_shape=outs,
        in_specs=[whole] * (3 + len(given)),
        out_specs=[whole] * len(outs),
        compiler_params=pltpu.CompilerParams(vmem_limit_bytes=16 << 20),
        cost_estimate=pl.CostEstimate(
            flops=2 * tokens * width * size * count,
            bytes_accessed=4 * tokens * size * count,
            transcendentals=0,
        ),
        name="shares",
    )(mixed, held, fetched, *given)


def over_lanes(part):
    everyone = jnp.broadcast_to(part[None], (lax.axis_size("tp"), *part.shape))
    return lax.all_to_all(everyone, "tp", 0, 0, tiled=True).sum(axis=0)


def fetched_rows(held):
    return lax.ppermute(held, "grp", [(i, i ^ 1) for i in range(lax.axis_size("grp"))])


def shards(hidden_in, in_gain, w_value, w_gate, conv_taps, norm_gain, norm_shift, w_out):
    layer_count = w_value.shape[0]
    reach_rows = conv_taps.shape[1] - 1
    tp = lax.axis_size("tp")
    tokens = hidden_in.shape[0]
    features = hidden_in.shape[1] * tp
    width = w_value.shape[2]
    channels = width * tp
    offsets = offsets_of(tp)

    half = w_out.shape[2] // 2
    mine = lax.axis_index("grp") % 2 * half
    taken = []
    for layer in range(layer_count):
        part = lax.dynamic_slice_in_dim(w_out[layer], mine, half, 1)
        rows = jnp.concatenate([w_value[layer], w_gate[layer], part], axis=1)
        taken.append(lax.all_gather(rows, "sp", axis=0, tiled=True))

    lead = -(-reach_rows // 32) * 32

    def run(layer, current):
        held = taken[layer][:, 2 * width :]
        fetched = fetched_rows(held)
        widened = current.astype(jnp.float32)
        scaled = (widened * in_gain[layer]).astype(jnp.bfloat16)
        near = [scaled if d == 0 else shifted(scaled, "tp", -d) for d in offsets]
        squares = over_lanes(jnp.sum(widened * widened, axis=1))
        inv_rms = lax.rsqrt(squares / features + epsilon)[:, None]
        far = [swapped(piece) for piece in near]
        gated = project(near[::-1] + far[::-1], inv_rms, taken[layer], width)
        conved = depthwise(gated, conv_taps[layer], lead)
        sums = jnp.stack([jnp.sum(conved, axis=1), jnp.sum(conved * conved, axis=1)])
        totals = over_lanes(sums)
        row_mean = totals[0] / channels
        spread = totals[1] / channels - row_mean * row_mean
        normed = (conved - row_mean[:, None]) * lax.rsqrt(spread + epsilon)[:, None] * norm_gain[
            layer
        ] + norm_shift[layer]
        mixed_out = jax.nn.silu(normed).astype(jnp.bfloat16)
        across = swapped(shares(mixed_out, held, fetched)[0])
        pairs, own = shares(mixed_out, held, fetched, across)
        summed = widened[lead:] + own
        for piece, d in zip(pairs, offsets):
            summed += shifted(piece, "tp", d).astype(jnp.float32)
        return summed.astype(jnp.bfloat16)

    ahead = lead * layer_count
    before = passed_along(hidden_in[tokens - ahead :], "sp", 1)
    current = jnp.concatenate([before, hidden_in], axis=0)
    for layer in range(layer_count):
        current = run(layer, current)
        ahead -= lead
        if ahead:
            absent = (jnp.arange(current.shape[0]) < ahead) & (lax.axis_index("sp") == 0)
            current = jnp.where(absent[:, None], 0, current)
    return current


def solution(mesh):
    placed = (
        P(("grp", "sp"), "tp"),
        P(None, "tp"),
        P(None, "sp", "tp"),
        P(None, "sp", "tp"),
        P(None, None, "tp"),
        P(None, "tp"),
        P(None, "tp"),
        P(None, "tp", "sp"),
    )
    return jax.shard_map(
        shards, mesh=mesh, in_specs=placed, out_specs=P(("grp", "sp"), "tp"), check_vma=False
    )
```

```python
import jax
import jax.numpy as jnp
from jax import lax
from jax.experimental import pallas as pl
from jax.experimental.pallas import tpu as pltpu
from jax.sharding import PartitionSpec as P

epsilon = 1e-06


def shifted(value, axis, steps):
    count = lax.axis_size(axis)
    return lax.ppermute(value, axis, [(i, (i + steps) % count) for i in range(count)])


def swapped(value):
    return lax.ppermute(value, "tp", [(i, i ^ 1) for i in range(lax.axis_size("tp"))])


def passed_along(value, axis, steps):
    count = lax.axis_size(axis)
    initial, last = (max(0, -steps), min(count, count - steps))
    return lax.ppermute(value, axis, [(source, source + steps) for source in range(initial, last)])


def offsets_of(count):
    half = count // 2
    apart = [d if d <= half else d - count for d in range(0, count, 2)]
    return sorted(apart, key=lambda d: -abs(d))


def project(pieces, inv_rms, rows, width):
    tokens, size = pieces[0].shape
    count = len(pieces)
    offsets = offsets_of(count)[::-1]

    def kernel(*refs):
        blocks, (inv_ref, w_ref, out_ref, near, held, near_in, held_in) = refs[:count], refs[count:]
        lane = lax.axis_index("tp")
        other = lane + 1 - 2 * (lane % 2)
        copies = []
        for i in range(count):
            base = lane if i < len(offsets) else other
            at = (base + offsets[i % len(offsets)] + count) % count
            rows_of = w_ref.at[pl.ds(pl.multiple_of(at * size, size), size), pl.ds(0, 2 * width)]
            copies.append(
                (
                    pltpu.make_async_copy(blocks[i], near.at[i], near_in.at[i]),
                    pltpu.make_async_copy(rows_of, held.at[i], held_in.at[i]),
                )
            )
            for copy in copies[-1]:
                copy.start()
        total = None
        for i in range(count):
            for copy in copies[i]:
                copy.wait()
            part = jnp.dot(near[i], held[i], preferred_element_type=jnp.float32)
            total = part if total is None else total + part
        inv = inv_ref[...]
        value, gate = total[:, :width] * inv, total[:, width:] * inv
        out_ref[...] = (value * jax.nn.sigmoid(gate)).astype(out_ref.dtype)

    whole = pl.BlockSpec(memory_space=pltpu.VMEM)
    apart = pl.BlockSpec(memory_space=pl.ANY)
    return pl.pallas_call(
        kernel,
        out_shape=jax.ShapeDtypeStruct((tokens, width), jnp.bfloat16),
        in_specs=[apart] * count + [whole, apart],
        out_specs=whole,
        scratch_shapes=[
            pltpu.VMEM((count, tokens, size), jnp.bfloat16),
            pltpu.VMEM((count, size, 2 * width), jnp.bfloat16),
            pltpu.SemaphoreType.DMA((count,)),
            pltpu.SemaphoreType.DMA((count,)),
        ],
        compiler_params=pltpu.CompilerParams(vmem_limit_bytes=50 << 20),
        cost_estimate=pl.CostEstimate(
            flops=4 * tokens * size * count * width,
            bytes_accessed=4 * size * count * width,
            transcendentals=tokens * width,
        ),
        name="project",
    )(*pieces, inv_rms, rows)


def depthwise(gated, taps, lead):
    total_rows, width = gated.shape
    tokens = total_rows - lead
    reach = taps.shape[0] - 1
    tile = 64 if tokens % 64 == 0 else 32
    lanes = 128

    def kernel(gated_ref, taps_ref, out_ref, wide):
        wide[...] = gated_ref[...].astype(jnp.float32)

        for start in range(0, tokens, tile):
            for lane in range(0, width, lanes):
                total = None
                for k in range(reach + 1):
                    window = wide[pl.ds(start + lead - reach + k, tile), pl.ds(lane, lanes)]
                    part = taps_ref[pl.ds(k, 1), pl.ds(lane, lanes)] * window
                    total = part if total is None else total + part
                out_ref[pl.ds(start, tile), pl.ds(lane, lanes)] = total

    whole = pl.BlockSpec(memory_space=pltpu.VMEM)
    return pl.pallas_call(
        kernel,
        out_shape=jax.ShapeDtypeStruct((tokens, width), jnp.float32),
        in_specs=[whole] * 2,
        out_specs=whole,
        scratch_shapes=[pltpu.VMEM((total_rows, width), jnp.float32)],
        compiler_params=pltpu.CompilerParams(vmem_limit_bytes=8 << 20),
        cost_estimate=pl.CostEstimate(
            flops=2 * tokens * width * (reach + 1),
            bytes_accessed=6 * tokens * width,
            transcendentals=0,
        ),
        name="depthwise",
    )(gated, taps)


def shares(mixed, held, fetched, across=None):
    tokens, width = mixed.shape
    tp = lax.axis_size("tp")
    offsets = offsets_of(tp)
    count = len(offsets)
    size = held.shape[0] // tp
    last = [] if across is None else [jax.ShapeDtypeStruct((tokens, size), jnp.float32)]
    outs = [jax.ShapeDtypeStruct((count - len(last), tokens, size), jnp.bfloat16)] + last

    def kernel(mixed_ref, held_ref, fetched_ref, *refs):
        arrived, (pairs_ref, *own_ref) = refs[: len(refs) - len(outs)], refs[len(refs) - len(outs) :]
        lane = lax.axis_index("tp")
        base = lane if arrived else lane + 1 - 2 * (lane % 2)
        odd = lax.axis_index("grp") % 2 == 1
        for i, d in enumerate(offsets):
            for j in range(0, size, width):
                at = pl.multiple_of((base + d + tp) % tp * size + j, width)
                block = held_ref[pl.ds(at, width), :]
                pair = fetched_ref[pl.ds(at, width), :]
                block = jnp.concatenate(
                    [jnp.where(odd, pair, block), jnp.where(odd, block, pair)], axis=1
                )
                part = jnp.dot(mixed_ref[...], block, preferred_element_type=jnp.float32)
                if arrived:
                    part += arrived[0][i, :, pl.ds(j, width)].astype(jnp.float32)
                if arrived and d == 0:
                    own_ref[0][:, pl.ds(j, width)] = part
                else:
                    pairs_ref[i, :, pl.ds(j, width)] = part.astype(jnp.bfloat16)

    whole = pl.BlockSpec(memory_space=pltpu.VMEM)
    given = [] if across is None else [across]
    return pl.pallas_call(
        kernel,
        out_shape=outs,
        in_specs=[whole] * (3 + len(given)),
        out_specs=[whole] * len(outs),
        compiler_params=pltpu.CompilerParams(vmem_limit_bytes=16 << 20),
        cost_estimate=pl.CostEstimate(
            flops=2 * tokens * width * size * count,
            bytes_accessed=4 * tokens * size * count,
            transcendentals=0,
        ),
        name="shares",
    )(mixed, held, fetched, *given)


def over_lanes(part):
    everyone = jnp.broadcast_to(part[None], (lax.axis_size("tp"), *part.shape))
    return lax.all_to_all(everyone, "tp", 0, 0, tiled=True).sum(axis=0)


def fetched_rows(held):
    return lax.ppermute(held, "grp", [(i, i ^ 1) for i in range(lax.axis_size("grp"))])


def shards(hidden_in, in_gain, w_value, w_gate, conv_taps, norm_gain, norm_shift, w_out):
    layer_count = w_value.shape[0]
    reach_rows = conv_taps.shape[1] - 1
    tp = lax.axis_size("tp")
    tokens = hidden_in.shape[0]
    features = hidden_in.shape[1] * tp
    width = w_value.shape[2]
    channels = width * tp
    offsets = offsets_of(tp)

    half = w_out.shape[2] // 2
    mine = lax.axis_index("grp") % 2 * half
    taken = []
    for layer in range(layer_count):
        part = lax.dynamic_slice_in_dim(w_out[layer], mine, half, 1)
        rows = jnp.concatenate([w_value[layer], w_gate[layer], part], axis=1)
        taken.append(lax.all_gather(rows, "sp", axis=0, tiled=True))

    lead = -(-reach_rows // 32) * 32

    def run(layer, current):
        held = taken[layer][:, 2 * width :]
        fetched = fetched_rows(held)
        widened = current.astype(jnp.float32)
        scaled = (widened * in_gain[layer]).astype(jnp.bfloat16)
        near = [scaled if d == 0 else shifted(scaled, "tp", -d) for d in offsets]
        squares = over_lanes(jnp.sum(widened * widened, axis=1))
        inv_rms = lax.rsqrt(squares / features + epsilon)[:, None]
        far = [swapped(piece) for piece in near]
        gated = project(near[::-1] + far[::-1], inv_rms, taken[layer], width)
        conved = depthwise(gated, conv_taps[layer], lead)
        sums = jnp.stack([jnp.sum(conved, axis=1), jnp.sum(conved * conved, axis=1)])
        totals = over_lanes(sums)
        row_mean = totals[0] / channels
        spread = totals[1] / channels - row_mean * row_mean
        normed = (conved - row_mean[:, None]) * lax.rsqrt(spread + epsilon)[:, None] * norm_gain[
            layer
        ] + norm_shift[layer]
        mixed_out = jax.nn.silu(normed).astype(jnp.bfloat16)
        across = swapped(shares(mixed_out, held, fetched)[0])
        pairs, own = shares(mixed_out, held, fetched, across)
        summed = widened[lead:] + own
        for piece, d in zip(pairs, offsets):
            summed += shifted(piece, "tp", d).astype(jnp.float32)
        return summed.astype(jnp.bfloat16)

    ahead = lead * layer_count
    before = passed_along(hidden_in[tokens - ahead :], "sp", 1)
    current = jnp.concatenate([before, hidden_in], axis=0)
    for layer in range(layer_count):
        current = run(layer, current)
        ahead -= lead
        if ahead:
            absent = (jnp.arange(current.shape[0]) < ahead) & (lax.axis_index("sp") == 0)
            current = jnp.where(absent[:, None], 0, current)
    return current


def solution(mesh):
    placed = (
        P(("grp", "sp"), "tp"),
        P(None, "tp"),
        P(None, "sp", "tp"),
        P(None, "sp", "tp"),
        P(None, None, "tp"),
        P(None, "tp"),
        P(None, "tp"),
        P(None, "tp", "sp"),
    )
    return jax.shard_map(
        shards, mesh=mesh, in_specs=placed, out_specs=P(("grp", "sp"), "tp"), check_vma=False
    )
```

```python
import jax
import jax.numpy as jnp
from jax import lax
from jax.experimental import pallas as pl
from jax.experimental.pallas import tpu as pltpu
from jax.sharding import PartitionSpec as P

epsilon = 1e-06


def shifted(value, axis, steps):
    count = lax.axis_size(axis)
    return lax.ppermute(value, axis, [(i, (i + steps) % count) for i in range(count)])


def swapped(value):
    return lax.ppermute(value, "tp", [(i, i ^ 1) for i in range(lax.axis_size("tp"))])


def passed_along(value, axis, steps):
    count = lax.axis_size(axis)
    initial, last = (max(0, -steps), min(count, count - steps))
    return lax.ppermute(value, axis, [(source, source + steps) for source in range(initial, last)])


def offsets_of(count):
    half = count // 2
    apart = [d if d <= half else d - count for d in range(0, count, 2)]
    return sorted(apart, key=lambda d: -abs(d))


def project(pieces, inv_rms, rows, width):
    stacked = not isinstance(pieces, list)
    count, (tokens, size) = len(pieces), pieces[0].shape
    offsets = offsets_of(count)[::-1]

    def kernel(*refs):
        *blocks, inv_ref, w_ref, out_ref, near, held, near_in, held_in = refs
        lane = lax.axis_index("tp")
        other = lane + 1 - 2 * (lane % 2)
        copies = []
        for i in range(count):
            base = lane if i < len(offsets) else other
            at = i if stacked else (base + offsets[i % len(offsets)] + count) % count
            block = blocks[0].at[i] if stacked else blocks[i]
            start = at * size if stacked else pl.multiple_of(at * size, size)
            rows_of = w_ref.at[pl.ds(start, size), pl.ds(0, 2 * width)]
            copies.append(
                (
                    pltpu.make_async_copy(block, near.at[i], near_in.at[i]),
                    pltpu.make_async_copy(rows_of, held.at[i], held_in.at[i]),
                )
            )
            for copy in copies[-1]:
                copy.start()
        total = None
        for i in range(count):
            for copy in copies[i]:
                copy.wait()
            part = jnp.dot(near[i], held[i], preferred_element_type=jnp.float32)
            total = part if total is None else total + part
        inv = inv_ref[...]
        value, gate = total[:, :width] * inv, total[:, width:] * inv
        out_ref[...] = (value * jax.nn.sigmoid(gate)).astype(out_ref.dtype)

    given = [pieces] if stacked else pieces
    whole = pl.BlockSpec(memory_space=pltpu.VMEM)
    apart = pl.BlockSpec(memory_space=pl.ANY)
    return pl.pallas_call(
        kernel,
        out_shape=jax.ShapeDtypeStruct((tokens, width), jnp.bfloat16),
        in_specs=[apart] * len(given) + [whole, apart],
        out_specs=whole,
        scratch_shapes=[
            pltpu.VMEM((count, tokens, size), jnp.bfloat16),
            pltpu.VMEM((count, size, 2 * width), jnp.bfloat16),
            pltpu.SemaphoreType.DMA((count,)),
            pltpu.SemaphoreType.DMA((count,)),
        ],
        compiler_params=pltpu.CompilerParams(vmem_limit_bytes=50 << 20),
        cost_estimate=pl.CostEstimate(
            flops=4 * tokens * size * count * width,
            bytes_accessed=4 * size * count * width,
            transcendentals=tokens * width,
        ),
        name="project",
    )(*given, inv_rms, rows)


def depthwise(gated, taps, lead):
    total_rows, width = gated.shape
    tokens = total_rows - lead
    reach = taps.shape[0] - 1
    tile = 64 if tokens % 64 == 0 else 32
    lanes = 128

    def kernel(gated_ref, taps_ref, out_ref, wide):
        wide[...] = gated_ref[...].astype(jnp.float32)

        for start in range(0, tokens, tile):
            for lane in range(0, width, lanes):
                total = None
                for k in range(reach + 1):
                    window = wide[pl.ds(start + lead - reach + k, tile), pl.ds(lane, lanes)]
                    part = taps_ref[pl.ds(k, 1), pl.ds(lane, lanes)] * window
                    total = part if total is None else total + part
                out_ref[pl.ds(start, tile), pl.ds(lane, lanes)] = total

    whole = pl.BlockSpec(memory_space=pltpu.VMEM)
    return pl.pallas_call(
        kernel,
        out_shape=jax.ShapeDtypeStruct((tokens, width), jnp.float32),
        in_specs=[whole] * 2,
        out_specs=whole,
        scratch_shapes=[pltpu.VMEM((total_rows, width), jnp.float32)],
        compiler_params=pltpu.CompilerParams(vmem_limit_bytes=8 << 20),
        cost_estimate=pl.CostEstimate(
            flops=2 * tokens * width * (reach + 1),
            bytes_accessed=6 * tokens * width,
            transcendentals=0,
        ),
        name="depthwise",
    )(gated, taps)


def shares(mixed, held, fetched, offsets, across=None):
    tokens, width = mixed.shape
    count = len(offsets)
    size = held.shape[0] // (2 * count)
    sent = count if across is None else sum(d != 0 for d in offsets)
    outs = [jax.ShapeDtypeStruct((sent, tokens, size), jnp.bfloat16)]
    outs += [jax.ShapeDtypeStruct((tokens, size), jnp.float32)] * (sent < count)
    given = [] if across is None else [across]

    def kernel(mixed_ref, held_ref, fetched_ref, *refs):
        arrived, (pairs_ref, *own_ref) = refs[: len(given)], refs[len(given) :]
        core = lax.axis_index("tp") % 2
        side = core if arrived else 1 - core
        odd = lax.axis_index("grp") % 2 == 1
        for i, d in enumerate(offsets):
            for j in range(0, size, width):
                at = pl.multiple_of((2 * i + side) * size + j, width)
                block = held_ref[pl.ds(at, width), :]
                pair = fetched_ref[pl.ds(at, width), :]
                block = jnp.concatenate(
                    [jnp.where(odd, pair, block), jnp.where(odd, block, pair)], axis=1
                )
                part = jnp.dot(mixed_ref[...], block, preferred_element_type=jnp.float32)
                if arrived:
                    part += arrived[0][i, :, pl.ds(j, width)].astype(jnp.float32)
                if arrived and d == 0:
                    own_ref[0][:, pl.ds(j, width)] = part
                else:
                    pairs_ref[i, :, pl.ds(j, width)] = part.astype(jnp.bfloat16)

    whole = pl.BlockSpec(memory_space=pltpu.VMEM)
    return pl.pallas_call(
        kernel,
        out_shape=outs,
        in_specs=[whole] * (3 + len(given)),
        out_specs=[whole] * len(outs),
        compiler_params=pltpu.CompilerParams(vmem_limit_bytes=16 << 20),
        cost_estimate=pl.CostEstimate(
            flops=2 * tokens * width * size * count,
            bytes_accessed=4 * tokens * size * count,
            transcendentals=0,
        ),
        name="shares",
    )(mixed, held, fetched, *given)


def over_lanes(part):
    everyone = jnp.broadcast_to(part[None], (lax.axis_size("tp"), *part.shape))
    return lax.all_to_all(everyone, "tp", 0, 0, tiled=True).sum(axis=0)


def fetched_rows(held):
    return lax.ppermute(held, "grp", [(i, i ^ 1) for i in range(lax.axis_size("grp"))])


def shards(hidden_in, in_gain, w_value, w_gate, conv_taps, norm_gain, norm_shift, w_out):
    layer_count = w_value.shape[0]
    reach_rows = conv_taps.shape[1] - 1
    tp = lax.axis_size("tp")
    tokens = hidden_in.shape[0]
    features = hidden_in.shape[1] * tp
    width = w_value.shape[2]
    channels = width * tp
    offsets = offsets_of(tp)

    half = w_out.shape[2] // 2
    mine = lax.axis_index("grp") % 2 * half
    taken = []
    for layer in range(layer_count):
        part = lax.dynamic_slice_in_dim(w_out[layer], mine, half, 1)
        rows = jnp.concatenate([w_value[layer], w_gate[layer], part], axis=1)
        taken.append(lax.all_gather(rows, "sp", axis=0, tiled=True))

    lead = -(-reach_rows // 32) * 32

    def run(layer, current):
        last = layer == layer_count - 1
        groups = [offsets[: tp // 4], offsets[tp // 4 :]] if last else [offsets]
        chip = 2 * (features // tp)
        held, fetched = [], []
        for group in groups:
            held.append(
                jnp.concatenate(
                    [
                        lax.dynamic_slice(
                            taken[layer],
                            ((lax.axis_index("tp") // 2 * 2 + d) % tp // 2 * chip, 2 * width),
                            (chip, half),
                        )
                        for d in group
                    ],
                    axis=0,
                )
            )
            fetched.append(fetched_rows(held[-1]))
        widened = current.astype(jnp.float32)
        scaled = (widened * in_gain[layer]).astype(jnp.bfloat16)
        if last:
            near = [scaled if d == 0 else shifted(scaled, "tp", -d) for d in offsets]
        else:
            everyone = jnp.broadcast_to(scaled[None], (tp, *scaled.shape))
            pieces = lax.all_to_all(everyone, "tp", 0, 0, tiled=True)
        squares = over_lanes(jnp.sum(widened * widened, axis=1))
        inv_rms = lax.rsqrt(squares / features + epsilon)[:, None]
        if last:
            pieces = near[::-1] + [swapped(piece) for piece in near[::-1]]
        gated = project(pieces, inv_rms, taken[layer], width)
        conved = depthwise(gated, conv_taps[layer], lead)
        sums = jnp.stack([jnp.sum(conved, axis=1), jnp.sum(conved * conved, axis=1)])
        totals = over_lanes(sums)
        row_mean = totals[0] / channels
        spread = totals[1] / channels - row_mean * row_mean
        normed = (conved - row_mean[:, None]) * lax.rsqrt(spread + epsilon)[:, None] * norm_gain[
            layer
        ] + norm_shift[layer]
        mixed_out = jax.nn.silu(normed).astype(jnp.bfloat16)
        summed = widened[lead:]
        for g, group in enumerate(groups):
            rows = (mixed_out, held[g], fetched[g], group)
            across = swapped(shares(*rows)[0])
            pairs, *own = shares(*rows, across)
            parts = own + [shifted(p, "tp", d) for p, d in zip(pairs, group)]
            for part in parts:
                summed += part.astype(jnp.float32)
        return summed.astype(jnp.bfloat16)

    ahead = lead * layer_count
    before = passed_along(hidden_in[tokens - ahead :], "sp", 1)
    current = jnp.concatenate([before, hidden_in], axis=0)
    for layer in range(layer_count):
        current = run(layer, current)
        ahead -= lead
        if ahead:
            absent = (jnp.arange(current.shape[0]) < ahead) & (lax.axis_index("sp") == 0)
            current = jnp.where(absent[:, None], 0, current)
    return current


def solution(mesh):
    placed = (
        P(("grp", "sp"), "tp"),
        P(None, "tp"),
        P(None, "sp", "tp"),
        P(None, "sp", "tp"),
        P(None, None, "tp"),
        P(None, "tp"),
        P(None, "tp"),
        P(None, "tp", "sp"),
    )
    return jax.shard_map(
        shards, mesh=mesh, in_specs=placed, out_specs=P(("grp", "sp"), "tp"), check_vma=False
    )
```

```python
import jax
import jax.numpy as jnp
from jax import lax
from jax.experimental import pallas as pl
from jax.experimental.pallas import tpu as pltpu
from jax.sharding import PartitionSpec as P

epsilon = 1e-06


def shifted(value, axis, steps):
    count = lax.axis_size(axis)
    return lax.ppermute(value, axis, [(i, (i + steps) % count) for i in range(count)])


def swapped(value):
    return lax.ppermute(value, "tp", [(i, i ^ 1) for i in range(lax.axis_size("tp"))])


def passed_along(value, axis, steps):
    count = lax.axis_size(axis)
    initial, last = (max(0, -steps), min(count, count - steps))
    return lax.ppermute(value, axis, [(source, source + steps) for source in range(initial, last)])


def offsets_of(count):
    half = count // 2
    apart = [d if d <= half else d - count for d in range(0, count, 2)]
    return sorted(apart, key=lambda d: -abs(d))


def project(pieces, inv_rms, rows, width):
    stacked = not isinstance(pieces, list)
    count, (tokens, size) = len(pieces), pieces[0].shape
    offsets = offsets_of(count)[::-1]

    def kernel(*refs):
        *blocks, inv_ref, w_ref, out_ref, near, held, near_in, held_in = refs
        lane = lax.axis_index("tp")
        other = lane + 1 - 2 * (lane % 2)
        copies = []
        for i in range(count):
            base = lane if i < len(offsets) else other
            at = i if stacked else (base + offsets[i % len(offsets)] + count) % count
            block = blocks[0].at[i] if stacked else blocks[i]
            start = at * size if stacked else pl.multiple_of(at * size, size)
            rows_of = w_ref.at[pl.ds(start, size), pl.ds(0, 2 * width)]
            copies.append(
                (
                    pltpu.make_async_copy(block, near.at[i], near_in.at[i]),
                    pltpu.make_async_copy(rows_of, held.at[i], held_in.at[i]),
                )
            )
            for copy in copies[-1]:
                copy.start()
        total = None
        for i in range(count):
            for copy in copies[i]:
                copy.wait()
            part = jnp.dot(near[i], held[i], preferred_element_type=jnp.float32)
            total = part if total is None else total + part
        inv = inv_ref[...]
        value, gate = total[:, :width] * inv, total[:, width:] * inv
        out_ref[...] = (value * jax.nn.sigmoid(gate)).astype(out_ref.dtype)

    given = [pieces] if stacked else pieces
    whole = pl.BlockSpec(memory_space=pltpu.VMEM)
    apart = pl.BlockSpec(memory_space=pl.ANY)
    return pl.pallas_call(
        kernel,
        out_shape=jax.ShapeDtypeStruct((tokens, width), jnp.bfloat16),
        in_specs=[apart] * len(given) + [whole, apart],
        out_specs=whole,
        scratch_shapes=[
            pltpu.VMEM((count, tokens, size), jnp.bfloat16),
            pltpu.VMEM((count, size, 2 * width), jnp.bfloat16),
            pltpu.SemaphoreType.DMA((count,)),
            pltpu.SemaphoreType.DMA((count,)),
        ],
        compiler_params=pltpu.CompilerParams(vmem_limit_bytes=50 << 20),
        cost_estimate=pl.CostEstimate(
            flops=4 * tokens * size * count * width,
            bytes_accessed=4 * size * count * width,
            transcendentals=tokens * width,
        ),
        name="project",
    )(*given, inv_rms, rows)


def depthwise(gated, taps, lead):
    total_rows, width = gated.shape
    tokens = total_rows - lead
    reach = taps.shape[0] - 1
    tile = 64 if tokens % 64 == 0 else 32
    lanes = 128

    def kernel(gated_ref, taps_ref, out_ref, wide):
        wide[...] = gated_ref[...].astype(jnp.float32)

        for start in range(0, tokens, tile):
            for lane in range(0, width, lanes):
                total = None
                for k in range(reach + 1):
                    window = wide[pl.ds(start + lead - reach + k, tile), pl.ds(lane, lanes)]
                    part = taps_ref[pl.ds(k, 1), pl.ds(lane, lanes)] * window
                    total = part if total is None else total + part
                out_ref[pl.ds(start, tile), pl.ds(lane, lanes)] = total

    whole = pl.BlockSpec(memory_space=pltpu.VMEM)
    return pl.pallas_call(
        kernel,
        out_shape=jax.ShapeDtypeStruct((tokens, width), jnp.float32),
        in_specs=[whole] * 2,
        out_specs=whole,
        scratch_shapes=[pltpu.VMEM((total_rows, width), jnp.float32)],
        compiler_params=pltpu.CompilerParams(vmem_limit_bytes=8 << 20),
        cost_estimate=pl.CostEstimate(
            flops=2 * tokens * width * (reach + 1),
            bytes_accessed=6 * tokens * width,
            transcendentals=0,
        ),
        name="depthwise",
    )(gated, taps)


def shares(mixed, held, fetched, offsets, across=None, parts=1):
    tokens, width = mixed.shape
    count = len(offsets)
    size = held.shape[0] // (2 * count)
    piece = size // parts
    if across is None:
        outs = [jax.ShapeDtypeStruct((count, tokens, size), jnp.bfloat16)]
    else:
        sent = parts * sum(d != 0 for d in offsets)
        outs = [jax.ShapeDtypeStruct((tokens, piece), jnp.bfloat16)] * sent
        outs += [jax.ShapeDtypeStruct((tokens, size), jnp.float32)] * (0 in offsets)
    given = [] if across is None else [across]

    def kernel(mixed_ref, held_ref, fetched_ref, *refs):
        arrived, out_refs = refs[: len(given)], refs[len(given) :]
        core = lax.axis_index("tp") % 2
        side = core if arrived else 1 - core
        odd = lax.axis_index("grp") % 2 == 1
        for i, d in enumerate(offsets):
            for j in range(0, size, width):
                at = pl.multiple_of((2 * i + side) * size + j, width)
                block = held_ref[pl.ds(at, width), :]
                pair = fetched_ref[pl.ds(at, width), :]
                block = jnp.concatenate(
                    [jnp.where(odd, pair, block), jnp.where(odd, block, pair)], axis=1
                )
                part = jnp.dot(mixed_ref[...], block, preferred_element_type=jnp.float32)
                if arrived:
                    part += arrived[0][i, :, pl.ds(j, width)].astype(jnp.float32)
                if arrived and d == 0:
                    out_refs[-1][:, pl.ds(j, width)] = part
                elif arrived:
                    into = out_refs[i * parts + j // piece]
                    into[:, pl.ds(j % piece, width)] = part.astype(jnp.bfloat16)
                else:
                    out_refs[0][i, :, pl.ds(j, width)] = part.astype(jnp.bfloat16)

    whole = pl.BlockSpec(memory_space=pltpu.VMEM)
    return pl.pallas_call(
        kernel,
        out_shape=outs,
        in_specs=[whole] * (3 + len(given)),
        out_specs=[whole] * len(outs),
        compiler_params=pltpu.CompilerParams(vmem_limit_bytes=16 << 20),
        cost_estimate=pl.CostEstimate(
            flops=2 * tokens * width * size * count,
            bytes_accessed=4 * tokens * size * count,
            transcendentals=0,
        ),
        name="shares",
    )(mixed, held, fetched, *given)


def joined(a, b):
    return (a.astype(jnp.float32) + b.astype(jnp.float32)).astype(jnp.bfloat16)


def over_lanes(part):
    everyone = jnp.broadcast_to(part[None], (lax.axis_size("tp"), *part.shape))
    return lax.all_to_all(everyone, "tp", 0, 0, tiled=True).sum(axis=0)


def fetched_rows(held):
    return lax.ppermute(held, "grp", [(i, i ^ 1) for i in range(lax.axis_size("grp"))])


def shards(hidden_in, in_gain, w_value, w_gate, conv_taps, norm_gain, norm_shift, w_out):
    layer_count = w_value.shape[0]
    reach_rows = conv_taps.shape[1] - 1
    tp = lax.axis_size("tp")
    tokens = hidden_in.shape[0]
    features = hidden_in.shape[1] * tp
    width = w_value.shape[2]
    channels = width * tp
    offsets = offsets_of(tp)

    half = w_out.shape[2] // 2
    mine = lax.axis_index("grp") % 2 * half
    taken = []
    for layer in range(layer_count):
        part = lax.dynamic_slice_in_dim(w_out[layer], mine, half, 1)
        rows = jnp.concatenate([w_value[layer], w_gate[layer], part], axis=1)
        taken.append(lax.all_gather(rows, "sp", axis=0, tiled=True))

    lead = -(-reach_rows // 32) * 32

    def run(layer, current):
        last = layer == layer_count - 1
        groups = [offsets[: tp // 4], offsets[tp // 4 :]] if last else [offsets]
        chip = 2 * (features // tp)
        held, fetched = [], []
        for group in groups:
            held.append(
                jnp.concatenate(
                    [
                        lax.dynamic_slice(
                            taken[layer],
                            ((lax.axis_index("tp") // 2 * 2 + d) % tp // 2 * chip, 2 * width),
                            (chip, half),
                        )
                        for d in group
                    ],
                    axis=0,
                )
            )
            fetched.append(fetched_rows(held[-1]))
        widened = current.astype(jnp.float32)
        scaled = (widened * in_gain[layer]).astype(jnp.bfloat16)
        if last:
            near = [scaled if d == 0 else shifted(scaled, "tp", -d) for d in offsets]
        else:
            everyone = jnp.broadcast_to(scaled[None], (tp, *scaled.shape))
            pieces = lax.all_to_all(everyone, "tp", 0, 0, tiled=True)
        squares = over_lanes(jnp.sum(widened * widened, axis=1))
        inv_rms = lax.rsqrt(squares / features + epsilon)[:, None]
        if last:
            pieces = near[::-1] + [swapped(piece) for piece in near[::-1]]
        gated = project(pieces, inv_rms, taken[layer], width)
        conved = depthwise(gated, conv_taps[layer], lead)
        sums = jnp.stack([jnp.sum(conved, axis=1), jnp.sum(conved * conved, axis=1)])
        stats = over_lanes(sums)
        row_mean = stats[0] / channels
        spread = stats[1] / channels - row_mean * row_mean
        normed = (conved - row_mean[:, None]) * lax.rsqrt(spread + epsilon)[:, None] * norm_gain[
            layer
        ] + norm_shift[layer]
        mixed_out = jax.nn.silu(normed).astype(jnp.bfloat16)
        totals = [widened[lead:]]
        for g, group in enumerate(groups):
            rows = (mixed_out, held[g], fetched[g], group)
            across = swapped(shares(*rows)[0])
            pairs = list(shares(*rows, across, 2 if last else 1))
            if 0 in group:
                totals.append(pairs.pop())
            if not last:
                totals += [shifted(p, "tp", d) for p, d in zip(pairs, group)]
            elif g == 0:
                far_up, far_down, up, up_free = pairs
                far_up, far_down = shifted(far_up, "tp", 2), shifted(far_down, "tp", -2)
                up_free = shifted(up_free, "tp", 2)
            else:
                down_free, down = pairs
                up = shifted(joined(up, far_up), "tp", 2)
                down = jnp.concatenate([down_free, joined(down, far_down)], axis=1)
                totals.append(shifted(down, "tp", -2))
                totals.append(jnp.concatenate([up, up_free], axis=1))
        summed = sum(part.astype(jnp.float32) for part in totals)
        return summed.astype(jnp.bfloat16)

    ahead = lead * layer_count
    before = passed_along(hidden_in[tokens - ahead :], "sp", 1)
    current = jnp.concatenate([before, hidden_in], axis=0)
    for layer in range(layer_count):
        current = run(layer, current)
        ahead -= lead
        if ahead:
            absent = (jnp.arange(current.shape[0]) < ahead) & (lax.axis_index("sp") == 0)
            current = jnp.where(absent[:, None], 0, current)
    return current


def solution(mesh):
    placed = (
        P(("grp", "sp"), "tp"),
        P(None, "tp"),
        P(None, "sp", "tp"),
        P(None, "sp", "tp"),
        P(None, None, "tp"),
        P(None, "tp"),
        P(None, "tp"),
        P(None, "tp", "sp"),
    )
    return jax.shard_map(
        shards, mesh=mesh, in_specs=placed, out_specs=P(("grp", "sp"), "tp"), check_vma=False
    )
```

```python
import jax
import jax.numpy as jnp
from jax import lax
from jax.experimental import pallas as pl
from jax.experimental.pallas import tpu as pltpu
from jax.sharding import PartitionSpec as P

epsilon = 1e-06


def shifted(value, axis, steps):
    count = lax.axis_size(axis)
    return lax.ppermute(value, axis, [(i, (i + steps) % count) for i in range(count)])


def swapped(value):
    return lax.ppermute(value, "tp", [(i, i ^ 1) for i in range(lax.axis_size("tp"))])


def passed_along(value, axis, steps):
    count = lax.axis_size(axis)
    initial, last = (max(0, -steps), min(count, count - steps))
    return lax.ppermute(value, axis, [(source, source + steps) for source in range(initial, last)])


def offsets_of(count):
    half = count // 2
    apart = [d if d <= half else d - count for d in range(0, count, 2)]
    return sorted(apart, key=lambda d: -abs(d))


def project(pieces, inv_rms, rows, width):
    stacked = not isinstance(pieces, list)
    count, (tokens, size) = len(pieces), pieces[0].shape
    offsets = offsets_of(count)[::-1]

    def kernel(*refs):
        *blocks, inv_ref, w_ref, out_ref, near, held, near_in, held_in = refs
        lane = lax.axis_index("tp")
        other = lane + 1 - 2 * (lane % 2)
        copies = []
        for i in range(count):
            base = lane if i < len(offsets) else other
            at = i if stacked else (base + offsets[i % len(offsets)] + count) % count
            block = blocks[0].at[i] if stacked else blocks[i]
            start = at * size if stacked else pl.multiple_of(at * size, size)
            rows_of = w_ref.at[pl.ds(start, size), pl.ds(0, 2 * width)]
            copies.append(
                (
                    pltpu.make_async_copy(block, near.at[i], near_in.at[i]),
                    pltpu.make_async_copy(rows_of, held.at[i], held_in.at[i]),
                )
            )
            for copy in copies[-1]:
                copy.start()
        total = None
        for i in range(count):
            for copy in copies[i]:
                copy.wait()
            part = jnp.dot(near[i], held[i], preferred_element_type=jnp.float32)
            total = part if total is None else total + part
        inv = inv_ref[...]
        value, gate = total[:, :width] * inv, total[:, width:] * inv
        out_ref[...] = (value * jax.nn.sigmoid(gate)).astype(out_ref.dtype)

    given = [pieces] if stacked else pieces
    whole = pl.BlockSpec(memory_space=pltpu.VMEM)
    apart = pl.BlockSpec(memory_space=pl.ANY)
    return pl.pallas_call(
        kernel,
        out_shape=jax.ShapeDtypeStruct((tokens, width), jnp.bfloat16),
        in_specs=[apart] * len(given) + [whole, apart],
        out_specs=whole,
        scratch_shapes=[
            pltpu.VMEM((count, tokens, size), jnp.bfloat16),
            pltpu.VMEM((count, size, 2 * width), jnp.bfloat16),
            pltpu.SemaphoreType.DMA((count,)),
            pltpu.SemaphoreType.DMA((count,)),
        ],
        compiler_params=pltpu.CompilerParams(vmem_limit_bytes=50 << 20),
        cost_estimate=pl.CostEstimate(
            flops=4 * tokens * size * count * width,
            bytes_accessed=4 * size * count * width,
            transcendentals=tokens * width,
        ),
        name="project",
    )(*given, inv_rms, rows)


def packed(layer, w_value, w_gate, w_out):
    depth, width = w_value.shape[1:]
    columns = w_out.shape[2]
    half = columns // 2

    def kernel(value_ref, gate_ref, out_ref, rows_ref):
        odd = lax.axis_index("grp") % 2 == 1
        rows_ref[:, pl.ds(0, width)] = value_ref[...]
        rows_ref[:, pl.ds(width, width)] = gate_ref[...]
        rows_ref[:, pl.ds(2 * width, half)] = jnp.where(
            odd, out_ref[:, pl.ds(half, half)], out_ref[:, pl.ds(0, half)]
        )

    def at(*shape):
        return pl.BlockSpec((None, *shape), lambda i: (layer, 0, 0))

    return pl.pallas_call(
        kernel,
        out_shape=jax.ShapeDtypeStruct((depth, 2 * width + half), w_value.dtype),
        grid=(1,),
        in_specs=[at(depth, width), at(depth, width), at(depth, columns)],
        out_specs=pl.BlockSpec((depth, 2 * width + half), lambda i: (0, 0)),
        compiler_params=pltpu.CompilerParams(vmem_limit_bytes=63 << 20),
        cost_estimate=pl.CostEstimate(
            flops=depth * width, bytes_accessed=10 * depth * width, transcendentals=0
        ),
        name="packed",
    )(w_value, w_gate, w_out)


def depthwise(gated, taps, lead):
    total_rows, width = gated.shape
    tokens = total_rows - lead
    reach = taps.shape[0] - 1
    tile = 64 if tokens % 64 == 0 else 32
    lanes = 128

    def kernel(gated_ref, taps_ref, out_ref, wide):
        wide[...] = gated_ref[...].astype(jnp.float32)

        for start in range(0, tokens, tile):
            for lane in range(0, width, lanes):
                total = None
                for k in range(reach + 1):
                    window = wide[pl.ds(start + lead - reach + k, tile), pl.ds(lane, lanes)]
                    part = taps_ref[pl.ds(k, 1), pl.ds(lane, lanes)] * window
                    total = part if total is None else total + part
                out_ref[pl.ds(start, tile), pl.ds(lane, lanes)] = total

    whole = pl.BlockSpec(memory_space=pltpu.VMEM)
    return pl.pallas_call(
        kernel,
        out_shape=jax.ShapeDtypeStruct((tokens, width), jnp.float32),
        in_specs=[whole] * 2,
        out_specs=whole,
        scratch_shapes=[pltpu.VMEM((total_rows, width), jnp.float32)],
        compiler_params=pltpu.CompilerParams(vmem_limit_bytes=8 << 20),
        cost_estimate=pl.CostEstimate(
            flops=2 * tokens * width * (reach + 1),
            bytes_accessed=6 * tokens * width,
            transcendentals=0,
        ),
        name="depthwise",
    )(gated, taps)


def shares(mixed, held, fetched, offsets, across=None, parts=1):
    tokens, width = mixed.shape
    count = len(offsets)
    size = held.shape[0] // (2 * count)
    piece = size // parts
    if across is None:
        outs = [jax.ShapeDtypeStruct((count, tokens, size), jnp.bfloat16)]
    else:
        sent = parts * sum(d != 0 for d in offsets)
        outs = [jax.ShapeDtypeStruct((tokens, piece), jnp.bfloat16)] * sent
        outs += [jax.ShapeDtypeStruct((tokens, size), jnp.float32)] * (0 in offsets)
    given = [] if across is None else [across]

    def kernel(mixed_ref, held_ref, fetched_ref, *refs):
        arrived, out_refs = refs[: len(given)], refs[len(given) :]
        core = lax.axis_index("tp") % 2
        side = core if arrived else 1 - core
        odd = lax.axis_index("grp") % 2 == 1
        for i, d in enumerate(offsets):
            for j in range(0, size, width):
                at = pl.multiple_of((2 * i + side) * size + j, width)
                block = held_ref[pl.ds(at, width), :]
                pair = fetched_ref[pl.ds(at, width), :]
                block = jnp.concatenate(
                    [jnp.where(odd, pair, block), jnp.where(odd, block, pair)], axis=1
                )
                part = jnp.dot(mixed_ref[...], block, preferred_element_type=jnp.float32)
                if arrived:
                    part += arrived[0][i, :, pl.ds(j, width)].astype(jnp.float32)
                if arrived and d == 0:
                    out_refs[-1][:, pl.ds(j, width)] = part
                elif arrived:
                    into = out_refs[i * parts + j // piece]
                    into[:, pl.ds(j % piece, width)] = part.astype(jnp.bfloat16)
                else:
                    out_refs[0][i, :, pl.ds(j, width)] = part.astype(jnp.bfloat16)

    whole = pl.BlockSpec(memory_space=pltpu.VMEM)
    return pl.pallas_call(
        kernel,
        out_shape=outs,
        in_specs=[whole] * (3 + len(given)),
        out_specs=[whole] * len(outs),
        compiler_params=pltpu.CompilerParams(vmem_limit_bytes=16 << 20),
        cost_estimate=pl.CostEstimate(
            flops=2 * tokens * width * size * count,
            bytes_accessed=4 * tokens * size * count,
            transcendentals=0,
        ),
        name="shares",
    )(mixed, held, fetched, *given)


def joined(a, b):
    return (a.astype(jnp.float32) + b.astype(jnp.float32)).astype(jnp.bfloat16)


def over_lanes(part):
    everyone = jnp.broadcast_to(part[None], (lax.axis_size("tp"), *part.shape))
    return lax.all_to_all(everyone, "tp", 0, 0, tiled=True).sum(axis=0)


def fetched_rows(held):
    return lax.ppermute(held, "grp", [(i, i ^ 1) for i in range(lax.axis_size("grp"))])


def shards(hidden_in, in_gain, w_value, w_gate, conv_taps, norm_gain, norm_shift, w_out):
    layer_count = w_value.shape[0]
    reach_rows = conv_taps.shape[1] - 1
    tp = lax.axis_size("tp")
    tokens = hidden_in.shape[0]
    features = hidden_in.shape[1] * tp
    width = w_value.shape[2]
    channels = width * tp
    offsets = offsets_of(tp)

    half = w_out.shape[2] // 2
    taken = []
    for layer in range(layer_count):
        rows = packed(layer, w_value, w_gate, w_out)
        taken.append(lax.all_gather(rows, "sp", axis=0, tiled=True))

    lead = -(-reach_rows // 32) * 32

    def run(layer, current):
        last = layer == layer_count - 1
        groups = [offsets[: tp // 4], offsets[tp // 4 :]] if last else [offsets]
        widened = current.astype(jnp.float32)
        scaled = (widened * in_gain[layer]).astype(jnp.bfloat16)
        if last:
            near = [scaled if d == 0 else shifted(scaled, "tp", -d) for d in offsets]
        else:
            everyone = jnp.broadcast_to(scaled[None], (tp, *scaled.shape))
            pieces = lax.all_to_all(everyone, "tp", 0, 0, tiled=True)
        squares = over_lanes(jnp.sum(widened * widened, axis=1))
        inv_rms = lax.rsqrt(squares / features + epsilon)
        lane, inv_rms = lax.optimization_barrier((lax.axis_index("tp") // 2 * 2, inv_rms))
        inv_rms = inv_rms[:, None]
        chip = 2 * (features // tp)
        held, fetched = [], []
        for group in groups:
            held.append(
                jnp.concatenate(
                    [
                        lax.dynamic_slice(
                            taken[layer],
                            ((lane + d) % tp // 2 * chip, 2 * width),
                            (chip, half),
                        )
                        for d in group
                    ],
                    axis=0,
                )
            )
            fetched.append(fetched_rows(held[-1]))
        if last:
            pieces = near[::-1] + [swapped(piece) for piece in near[::-1]]
        gated = project(pieces, inv_rms, taken[layer], width)
        conved = depthwise(gated, conv_taps[layer], lead)
        sums = jnp.stack([jnp.sum(conved, axis=1), jnp.sum(conved * conved, axis=1)])
        stats = over_lanes(sums)
        row_mean = stats[0] / channels
        spread = stats[1] / channels - row_mean * row_mean
        normed = (conved - row_mean[:, None]) * lax.rsqrt(spread + epsilon)[:, None] * norm_gain[
            layer
        ] + norm_shift[layer]
        mixed_out = jax.nn.silu(normed).astype(jnp.bfloat16)
        totals = [widened[lead:]]
        for g, group in enumerate(groups):
            rows = (mixed_out, held[g], fetched[g], group)
            across = swapped(shares(*rows)[0])
            pairs = list(shares(*rows, across, 2 if last else 1))
            if 0 in group:
                totals.append(pairs.pop())
            if not last:
                totals += [shifted(p, "tp", d) for p, d in zip(pairs, group)]
            elif g == 0:
                far_up, far_down, up, up_free = pairs
                far_up, far_down = shifted(far_up, "tp", 2), shifted(far_down, "tp", -2)
                up_free = shifted(up_free, "tp", 2)
            else:
                down_free, down = pairs
                up = shifted(joined(up, far_up), "tp", 2)
                down = jnp.concatenate([down_free, joined(down, far_down)], axis=1)
                totals.append(shifted(down, "tp", -2))
                totals.append(jnp.concatenate([up, up_free], axis=1))
        summed = sum(part.astype(jnp.float32) for part in totals)
        return summed.astype(jnp.bfloat16)

    ahead = lead * layer_count
    before = passed_along(hidden_in[tokens - ahead :], "sp", 1)
    current = jnp.concatenate([before, hidden_in], axis=0)
    for layer in range(layer_count):
        current = run(layer, current)
        ahead -= lead
        if ahead:
            absent = (jnp.arange(current.shape[0]) < ahead) & (lax.axis_index("sp") == 0)
            current = jnp.where(absent[:, None], 0, current)
    return current


def solution(mesh):
    placed = (
        P(("grp", "sp"), "tp"),
        P(None, "tp"),
        P(None, "sp", "tp"),
        P(None, "sp", "tp"),
        P(None, None, "tp"),
        P(None, "tp"),
        P(None, "tp"),
        P(None, "tp", "sp"),
    )
    return jax.shard_map(
        shards, mesh=mesh, in_specs=placed, out_specs=P(("grp", "sp"), "tp"), check_vma=False
    )
```
